32 devices in a mesh: kv: 4 (over y, x), tp: 8 (over z, core).
Axes of the slice: x: 2, y: 2, z: 4, core: 2. Of those that a mesh axis runs over, the one named last changes fastest.
Arguments:
- tokens: bfloat16 [128, 4096], P(None, 'tp'), may hold values from -6 to 6
- norm_gain: float32 [4096], P('tp'), may hold values from 0.1 to 1.9
- query_weight: bfloat16 [4096, 2048], P('tp', 'kv'), may hold values from -0.09375 to 0.09375
- key_weight: bfloat16 [4096, 2048], P('tp', 'kv'), may hold values from -0.09375 to 0.09375
- value_weight: bfloat16 [4096, 2048], P('tp', 'kv'), may hold values from -0.09375 to 0.09375
- input_gate_weight: bfloat16 [4096, 16], P('tp'), may hold values from -0.09375 to 0.09375
- forget_gate_weight: bfloat16 [4096, 16], P('tp'), may hold values from -0.09375 to 0.09375
- input_gate_bias: float32 [16], P('kv'), may hold values from -2 to 2
- forget_gate_bias: float32 [16], P('kv'), may hold values from 1 to 6
- memory_state: float32 [128, 16, 128, 128], P('tp', 'kv'), may hold values from -12 to 12
- normalizer_state: float32 [128, 16, 128], P('tp', 'kv'), may hold values from -24 to 24
- stabilizer_state: float32 [128, 16], P('tp', 'kv'), may hold values from -1 to 3
- block_keys: bfloat16 [128, 16, 128, 128], P('tp', 'kv'), may hold values from -6 to 6
- block_values: bfloat16 [128, 16, 128, 128], P('tp', 'kv'), may hold values from -6 to 6
- block_input_pre: float32 [128, 16, 128], P('tp', 'kv'), may hold values from -6 to 6
- block_forget_pre: float32 [128, 16, 128], P('tp', 'kv'), may hold values from -6 to 6
- block_lengths: int32 [128], P('tp'), may hold values from 1 to 128, 6553 in all
- head_norm_gain: float32 [2048], P('kv'), may hold values from 0.1 to 1.9
- output_weight: bfloat16 [2048, 4096], P('kv', 'tp'), may hold values from -0.125 to 0.125
- mixer_norm_gain: float32 [4096], P('tp'), may hold values from 0.1 to 1.9
- gate_weight: bfloat16 [4096, 11264], P('tp', 'kv'), may hold values from -0.09375 to 0.09375
- up_weight: bfloat16 [4096, 11264], P('tp', 'kv'), may hold values from -0.09375 to 0.09375
- down_weight: bfloat16 [11264, 4096], P('kv', 'tp'), may hold values from -0.0546875 to 0.0546875
Outputs:
- layer_output: float32 [128, 4096], P(None, 'tp')
The draws below stay inside these ranges and needn't reach their ends.
Inputs may be any that keep to these rules, and one draw needn't show every extreme that they name: `block_lengths`: some sequence has exactly 128 live positions.
All inputs are finite; a program needn't handle non-finite values. No bound on the sum of `block_lengths` on one device may be relied on, other than what follows from the above.
Results may differ from the reference program's by a relative error of at most 0.0078.
Values may be sent and summed in bfloat16 or wider, within the bound.
A program may use at most 64 MiB of HBM per device.

```python
import math
import jax
import jax.numpy as jnp
import numpy as np
from jax import lax

D = 4096
H = 16
DH = 128
FF = 11264
BLK = 128
WIDTH = 2048
SEQS = 128


def block_levels(own_key, extent, cuts, least, high):
    loudness = 1.0
    for axis_at, blocks in cuts:
        draws = jax.random.uniform(jax.random.fold_in(jax.random.fold_in(own_key, 6), axis_at), (blocks,), jnp.float32, least / len(cuts), high / len(cuts))
        loudness = loudness * jnp.repeat(jnp.exp(draws), extent[axis_at] // blocks).reshape((-1,) + (1,) * (len(extent) - 1 - axis_at))
    return loudness


def length_profile(number_of, total, reach, lean):
    loads = [(1 << 20) // math.isqrt(grade ** lean) + 1 for grade in range(2, number_of + 1)]
    rest, holding = total - reach - (number_of - 1), [1] * (number_of - 1)
    while rest > 0:
        free = [i for i in range(number_of - 1) if holding[i] < reach]
        whole, remaining = sum([loads[i] for i in free]), rest
        for i in free:
            more = min(reach - holding[i], max(1, remaining * loads[i] // whole), rest)
            holding[i] = holding[i] + more
            rest = rest - more
    return np.array([reach] + holding)


def uneven_parts(own_key, number_of, total, reach, skew):
    if number_of == 2:
        one = jax.random.randint(own_key, (), max(1, total - reach), min(reach, total - 1) + 1)
        return jnp.stack([one, total - one])
    tallies = jnp.asarray(length_profile(number_of, total, reach, skew), jnp.int32)
    pairs = (number_of - 1) // 2
    giver, receiver = tallies[1:1 + 2 * pairs:2], tallies[2:2 + 2 * pairs:2]
    room = jnp.minimum(giver - 1, reach - receiver)
    shifted = jax.random.randint(jax.random.fold_in(own_key, 1), (pairs,), 0, 1 << 20) % (room + 1)
    tallies = tallies.at[1:1 + 2 * pairs:2].set(giver - shifted).at[2:2 + 2 * pairs:2].set(receiver + shifted)
    return tallies[jax.random.permutation(jax.random.fold_in(own_key, 2), number_of)]


def centred(key, shape, scale, most, shards=(), dtype=jnp.bfloat16):
    level = block_levels(key, shape, shards, -0.22, 0.18) if shards else 1.0
    entries = jax.random.normal(key, shape, jnp.float32) * scale * level
    return jnp.minimum(jnp.maximum(entries, -most), most).astype(dtype)


def setup_inputs(seed: int = 0) -> dict:
    streams_of = jax.random.split(jax.random.key(seed), 24)
    return {
        "tokens": centred(streams_of[0], (SEQS, D), 1.0, 6.0, ((1, 8),)),
        "norm_gain": jnp.clip(1.0 + 0.18 * jax.random.normal(streams_of[1], (D,), jnp.float32), 0.1, 1.9),
        "query_weight": centred(streams_of[2], (D, WIDTH), D ** -0.5, 0.09375, ((0, 8), (1, 4))),
        "key_weight": centred(streams_of[3], (D, WIDTH), D ** -0.5, 0.09375, ((0, 8), (1, 4))),
        "value_weight": centred(streams_of[4], (D, WIDTH), D ** -0.5, 0.09375, ((0, 8), (1, 4))),
        "input_gate_weight": centred(streams_of[5], (D, H), D ** -0.5, 0.09375, ((0, 8),)),
        "forget_gate_weight": centred(streams_of[6], (D, H), D ** -0.5, 0.09375, ((0, 8),)),
        "input_gate_bias": jnp.clip(jax.random.uniform(streams_of[7], (H,), jnp.float32, -2.0, 2.0) * block_levels(streams_of[7], (H,), ((0, 4),), -0.4, 0.0), -2.0, 2.0),
        "forget_gate_bias": jnp.clip(1.0 + 5.0 * jax.random.uniform(streams_of[8], (H,), jnp.float32) ** block_levels(streams_of[8], (H,), ((0, 4),), -0.2, 0.2), 1.0, 6.0),
        "memory_state": centred(streams_of[9], (SEQS, H, DH, DH), 2.0, 12.0, ((0, 8), (1, 4)), jnp.float32),
        "normalizer_state": centred(streams_of[10], (SEQS, H, DH), 4.0, 24.0, ((0, 8), (1, 4)), jnp.float32),
        "stabilizer_state": jnp.clip(-1.0 + 4.0 * jax.random.uniform(streams_of[11], (SEQS, H), jnp.float32) ** block_levels(streams_of[11], (SEQS, H), ((0, 8), (1, 4)), -0.2, 0.2), -1.0, 3.0),
        "block_keys": centred(streams_of[12], (SEQS, H, BLK, DH), 1.0, 6.0, ((0, 8), (1, 4))),
        "block_values": centred(streams_of[13], (SEQS, H, BLK, DH), 1.0, 6.0, ((0, 8), (1, 4))),
        "block_input_pre": centred(streams_of[14], (SEQS, H, BLK), 1.0, 6.0, ((0, 8), (1, 4)), jnp.float32),
        "block_forget_pre": centred(streams_of[15], (SEQS, H, BLK), 1.0, 6.0, ((0, 8), (1, 4)), jnp.float32),
        "block_lengths": uneven_parts(streams_of[16], SEQS, SEQS * BLK * 2 // 5, BLK, 2).astype(jnp.int32),
        "head_norm_gain": jnp.clip(1.0 + 0.18 * jax.random.normal(streams_of[17], (WIDTH,), jnp.float32), 0.1, 1.9),
        "output_weight": centred(streams_of[18], (WIDTH, D), WIDTH ** -0.5, 0.125, ((0, 4), (1, 8))),
        "mixer_norm_gain": jnp.clip(1.0 + 0.18 * jax.random.normal(streams_of[19], (D,), jnp.float32), 0.1, 1.9),
        "gate_weight": centred(streams_of[20], (D, FF), D ** -0.5, 0.09375, ((0, 8), (1, 4))),
        "up_weight": centred(streams_of[21], (D, FF), D ** -0.5, 0.09375, ((0, 8), (1, 4))),
        "down_weight": centred(streams_of[22], (FF, D), FF ** -0.5, 0.0546875, ((0, 4), (1, 8))),
    }


epsilon = 1e-06

def memory_cell(queries, new_keys, new_values, log_input, log_forget, memory, normalizer, stabilizer, cached_keys, cached_values, input_pre, forget_pre, lengths, input_bias, forget_bias):
    positions = jnp.arange(cached_keys.shape[2])
    is_live = (positions[None, :] < lengths[:, None])[:, None, :]
    cached_input = input_pre + input_bias[None, :, None]
    cached_forget = jnp.where(is_live, jax.nn.log_sigmoid(forget_pre + forget_bias[None, :, None]), 0.0)
    after_mask = (positions[:, None] > positions[None, :]).astype(jnp.float32)
    later_forget = jnp.einsum('bhu,us->bhs', cached_forget, after_mask, precision=lax.Precision.HIGHEST) + log_forget[..., None]
    total_forget = lax.optimization_barrier(jnp.sum(cached_forget, axis=-1)) + log_forget
    exponent = jnp.where(is_live, later_forget + cached_input, -jnp.inf)
    carried = total_forget + stabilizer
    stab_max = jnp.maximum(jnp.maximum(lax.optimization_barrier(jnp.max(exponent, axis=-1)), carried), log_input)
    query_wide = queries.astype(jnp.float32)
    scores = jnp.einsum('bhd,bhsd->bhs', query_wide, cached_keys.astype(jnp.float32))
    block_weight = jnp.exp(exponent - stab_max[..., None]) * scores
    block_probs = block_weight.astype(jnp.bfloat16)
    block_sum = jnp.einsum('bhs,bhsd->bhd', block_probs.astype(jnp.float32), cached_values.astype(jnp.float32))
    new_weight = jnp.exp(log_input - stab_max) * lax.optimization_barrier(jnp.sum(query_wide * new_keys.astype(jnp.float32), axis=-1))
    state_weight = jnp.exp(carried - stab_max)
    state_sum = jnp.einsum('bhkv,bhk->bhv', memory, query_wide, precision=lax.Precision.HIGHEST)
    state_norm = lax.optimization_barrier(jnp.sum(normalizer * query_wide, axis=-1))
    numerator = block_sum + new_weight[..., None] * new_values.astype(jnp.float32) + state_weight[..., None] * state_sum
    denominator = lax.optimization_barrier(jnp.sum(block_weight, axis=-1)) + new_weight + state_weight * state_norm
    return numerator / jnp.maximum(jnp.abs(denominator), 1.0)[..., None]

def head_scale(cell_out, gain):
    return (cell_out * gain.reshape(cell_out.shape[1], cell_out.shape[2])).astype(jnp.bfloat16)

def reference(tokens, norm_gain, query_weight, key_weight, value_weight, input_gate_weight, forget_gate_weight, input_gate_bias, forget_gate_bias, memory_state, normalizer_state, stabilizer_state, block_keys, block_values, block_input_pre, block_forget_pre, block_lengths, head_norm_gain, output_weight, mixer_norm_gain, gate_weight, up_weight, down_weight):
    seq_rows = tokens.shape[0]
    tok_wide = tokens.astype(jnp.float32)
    first_scale = lax.rsqrt(lax.optimization_barrier(jnp.mean(tok_wide * tok_wide, axis=1)) + epsilon)[:, None]
    scaled_in = (tok_wide * norm_gain).astype(jnp.bfloat16)

    def project(weight):
        return jnp.dot(scaled_in, weight, preferred_element_type=jnp.float32) * first_scale
    queries = (project(query_weight) * DH ** (-0.5)).astype(jnp.bfloat16).reshape(seq_rows, H, DH)
    new_keys = project(key_weight).astype(jnp.bfloat16).reshape(seq_rows, H, DH)
    new_values = project(value_weight).astype(jnp.bfloat16).reshape(seq_rows, H, DH)
    log_input = project(input_gate_weight) + input_gate_bias
    log_forget = jax.nn.log_sigmoid(project(forget_gate_weight) + forget_gate_bias)
    cell_out = memory_cell(queries, new_keys, new_values, log_input, log_forget, memory_state, normalizer_state, stabilizer_state, block_keys, block_values, block_input_pre, block_forget_pre, block_lengths, input_gate_bias, forget_gate_bias)
    head_out = head_scale(cell_out, head_norm_gain).reshape(seq_rows, H * DH)
    attended = jnp.dot(head_out, output_weight, preferred_element_type=jnp.float32)
    res_wide = tok_wide + attended
    second_scale = lax.rsqrt(lax.optimization_barrier(jnp.mean(res_wide * res_wide, axis=1)) + epsilon)[:, None]
    mid_scaled = (res_wide * mixer_norm_gain).astype(jnp.bfloat16)
    gate_pre = jnp.dot(mid_scaled, gate_weight, preferred_element_type=jnp.float32) * second_scale
    up_pre = jnp.dot(mid_scaled, up_weight, preferred_element_type=jnp.float32) * second_scale
    hidden = (jax.nn.silu(gate_pre) * up_pre).astype(jnp.bfloat16)
    mixed = jnp.dot(hidden, down_weight, preferred_element_type=jnp.float32)
    return res_wide + mixed
```

```python
import functools

import jax
import jax.numpy as jnp
from jax import lax
from jax.experimental import pallas as pl
from jax.experimental.pallas import tpu as pltpu
from jax.sharding import PartitionSpec as P

epsilon = 1e-06
MESH = pl.DeviceIdType.MESH
F32, BF16 = jnp.float32, jnp.bfloat16


def log_sigmoid(x):
    return -(jnp.maximum(-x, 0.0) + jnp.log1p(jnp.exp(-jnp.abs(x))))


def dot32(a, b):
    return jnp.dot(a, b, preferred_element_type=F32)


def dot_t(a, b):
    return lax.dot_general(a, b, (((1,), (1,)), ((), ())), preferred_element_type=F32)


class Ring:
    def __init__(self, n_tp, n_kv):
        self.n_tp, self.n_kv, self.nz = n_tp, n_kv, n_tp // 2
        self.t = lax.axis_index("tp")
        self.kv = lax.axis_index("kv")
        self.core = lax.rem(self.t, 2)
        self.z = lax.div(self.t, 2)
        self.partner = self.z * 2 + (1 - self.core)

    def up(self, k):
        return lax.rem(self.z + k, self.nz)

    def down(self, k):
        return lax.rem(self.z + (self.nz - k), self.nz)

    def same(self, z):
        return z * 2 + self.core

    def other(self, z):
        return z * 2 + (1 - self.core)


def remote(src, dst, send, recv, **device):
    return pltpu.make_async_remote_copy(
        src_ref=src, dst_ref=dst, send_sem=send, recv_sem=recv,
        device_id=device, device_id_type=MESH,
    )


class ReduceScatter:
    def __init__(self, ring, sb, rb1, sb2, rb2, sems):
        self.g, self.sb, self.rb1, self.sb2, self.rb2 = ring, sb, rb1, sb2, rb2
        self.s1, self.r1, self.s2, self.r2 = sems

    def pair(self, z):
        g = self.g
        return remote(self.sb.at[g.other(z)], self.rb1.at[z], self.s1.at[z], self.r1.at[z], tp=g.partner)

    def along(self, k):
        g = self.g
        return remote(self.sb2.at[k], self.rb2.at[k], self.s2.at[k], self.r2.at[k], tp=g.same(g.up(k)))

    def order(self):
        return list(range(1, self.g.nz)) + [0]

    def start(self):
        for k in self.order():
            self.pair(self.g.up(k)).start()

    def middle(self):
        g = self.g
        for k in self.order():
            z = g.up(k)
            self.pair(z).wait_recv()
            if k:
                both = self.sb[g.same(z)].astype(F32) + self.rb1[z].astype(F32)
                self.sb2[k] = both.astype(self.sb2.dtype)
                self.along(k).start()

    def end(self):
        g = self.g
        for k in range(1, g.nz):
            self.along(k).wait_recv()
        total = self.sb[g.t].astype(F32) + self.rb1[g.z].astype(F32)
        for k in range(1, g.nz):
            total = total + self.rb2[k].astype(F32)
        return total

    def drain(self):
        for k in range(self.g.nz):
            self.pair(k).wait_send()
        for k in range(1, self.g.nz):
            self.along(k).wait_send()


class Gather:
    def __init__(self, ring, buf, sems):
        self.g, self.buf = ring, buf
        self.s, self.f, self.r = sems

    def direct(self, k):
        g = self.g
        return remote(self.buf.at[g.t], self.buf.at[g.t], self.s.at[k], self.r.at[g.t], tp=g.same(g.up(k)))

    def pass_on(self, block, k):
        g = self.g
        return remote(self.buf.at[block], self.buf.at[block], self.f.at[k], self.r.at[block], tp=g.partner)

    def run(self):
        g = self.g
        for k in range(1, g.nz):
            self.direct(k).start()
        self.pass_on(g.t, 0).start()
        for k in range(1, g.nz):
            copy = self.pass_on(g.same(g.down(k)), k)
            copy.wait_recv()
            copy.start()
        for k in range(g.nz):
            self.pass_on(g.other(g.down(k)), k).wait_recv()

    def drain(self):
        g = self.g
        for k in range(1, g.nz):
            self.direct(k).wait_send()
        for k in range(g.nz):
            self.pass_on(g.same(g.down(k)), k).wait_send()


class SumOverKv:
    def __init__(self, ring, sb, rb, out, sems):
        self.g, self.sb, self.rb, self.out = ring, sb, rb, out
        self.s1, self.r1, self.s2, self.r2 = sems

    def peer(self, k):
        return lax.rem(self.g.kv + k, self.g.n_kv)

    def part(self, k):
        p = self.peer(k)
        return remote(self.sb.at[p], self.rb.at[k], self.s1.at[k], self.r1.at[k], kv=p)

    def share(self, k, block):
        return remote(self.out.at[block], self.out.at[block], self.s2.at[k], self.r2.at[block], kv=self.peer(k))

    def run(self):
        n, me = self.g.n_kv, self.g.kv
        for k in range(1, n):
            self.part(k).start()
        total = self.sb[me].astype(F32)
        for k in range(1, n):
            self.part(k).wait_recv()
            total = total + self.rb[k].astype(F32)
        self.out[me] = total.astype(self.out.dtype)
        for k in range(1, n):
            self.share(k, me).start()
        for k in range(1, n):
            self.share(k, self.peer(k)).wait_recv()

    def drain(self):
        for k in range(1, self.g.n_kv):
            self.part(k).wait_send()
            self.share(k, self.g.kv).wait_send()


NAMES = (
    "tokens", "norm_gain", "wq", "wk", "wv", "wi", "wf", "bi", "bf", "mem", "nrm", "stab",
    "keys", "vals", "ipre", "fpre", "lens", "hgain", "wo", "mgain", "wg", "wu", "wd",
)
HELD = ("keys", "mem", "vals", "wo", "wg", "wu", "wd")


def kernel(n_tp, n_kv, model, scratch_names, *refs):
    ins = dict(zip(NAMES, refs))
    out = refs[len(NAMES)]
    sc = dict(zip(scratch_names, refs[len(NAMES) + 1:]))
    g = Ring(n_tp, n_kv)
    rows, feats = ins["tokens"].shape
    r, heads, block, size = ins["keys"].shape
    width = heads * size
    every = ins["wi"].shape[1]

    loads = {}
    for i, name in enumerate(HELD):
        loads[name] = pltpu.make_async_copy(ins[name], sc["v_" + name], sc["load_sem"].at[i])
        loads[name].start()

    barrier = pltpu.get_barrier_semaphore()
    for k in range(1, g.nz):
        pl.semaphore_signal(barrier, inc=1, device_id={"tp": g.same(g.up(k))}, device_id_type=MESH)
    pl.semaphore_signal(barrier, inc=1, device_id={"tp": g.partner}, device_id_type=MESH)
    for k in range(1, n_kv):
        pl.semaphore_signal(barrier, inc=1, device_id={"kv": lax.rem(g.kv + k, n_kv)}, device_id_type=MESH)

    def rs(name):
        parts = [sc[f"{name}_{p}"] for p in ("sb", "rb1", "sb2", "rb2")]
        sems = [sc[f"{name}_{p}"] for p in ("s1", "r1", "s2", "r2")]
        return ReduceScatter(g, *parts, sems)

    wide = ins["tokens"][...].astype(F32)
    scaled = (wide * ins["norm_gain"][...]).astype(BF16)
    small_sb = sc["small_sb"]
    small_sb[:, :, 0:every] = dot32(scaled, ins["wi"][...]).reshape(n_tp, r, every)
    small_sb[:, :, every:2 * every] = dot32(scaled, ins["wf"][...]).reshape(n_tp, r, every)
    small_sb[:, :, 2 * every:2 * every + 1] = jnp.sum(wide * wide, axis=1, keepdims=True).reshape(n_tp, r, 1)
    qkv_sb = sc["qkv_sb"]
    for i, name in enumerate(("wq", "wk", "wv")):
        qkv_sb[:, :, i * width:(i + 1) * width] = (
            dot32(scaled, ins[name][...]).astype(BF16).reshape(n_tp, r, width)
        )
    pl.semaphore_wait(barrier, g.nz + n_kv - 1)
    small, qkv = rs("small"), rs("qkv")
    small.start()
    qkv.start()
    small.middle()
    qkv.middle()

    row_of = lax.broadcasted_iota(jnp.int32, (r, block), 0)
    position = lax.broadcasted_iota(jnp.int32, (r, block), 1)
    length = jnp.zeros((r, block), jnp.int32)
    for b in range(r):
        length = jnp.where(row_of == b, ins["lens"][b], length)
    live = position < length
    before = lax.broadcasted_iota(jnp.int32, (block, block), 0)
    after_mask = (before > lax.broadcasted_iota(jnp.int32, (block, block), 1)).astype(F32)
    later, whole_forget, cached_in = [], [], []
    for h in range(heads):
        cached = jnp.where(live, log_sigmoid(ins["fpre"][:, h, :] + ins["bf"][h]), 0.0)
        later.append(
            jnp.dot(cached, after_mask, precision=lax.Precision.HIGHEST, preferred_element_type=F32)
        )
        whole_forget.append(jnp.sum(cached, axis=-1, keepdims=True))
        cached_in.append(ins["ipre"][:, h, :] + ins["bi"][h])

    sums = small.end()
    square = sums[:, 2 * every:2 * every + 1]
    scale = lax.rsqrt(square / model + epsilon)
    lane = lax.broadcasted_iota(jnp.int32, sums.shape, 1)

    def column(at):
        return jnp.sum(jnp.where(lane == at, sums, 0.0), axis=-1, keepdims=True)

    projected = qkv.end() * scale
    query = (projected[:, :width] * size ** (-0.5)).astype(BF16)
    new_key = projected[:, width:2 * width].astype(BF16).astype(F32)
    new_value = projected[:, 2 * width:].astype(BF16).astype(F32)

    loads["keys"].wait()
    loads["mem"].wait()
    q_of = [query[:, h * size:(h + 1) * size] for h in range(heads)]
    row_v = lax.broadcasted_iota(jnp.int32, (r, size), 0)
    group = 4 if r % 4 == 0 else 1

    def scan_keys(i, carry):
        scores, states = list(carry[0]), list(carry[1])
        for j in range(group):
            b = i * group + j
            for h in range(heads):
                s = dot_t(q_of[h], sc["v_keys"][b, h])
                m = dot32(q_of[h], sc["v_mem"][b, h].astype(BF16))
                scores[h] = jnp.where(row_of == b, s, scores[h])
                states[h] = jnp.where(row_v == b, m, states[h])
        return tuple(scores), tuple(states)

    none_s = tuple(jnp.zeros((r, block), F32) for _ in range(heads))
    none_v = tuple(jnp.zeros((r, size), F32) for _ in range(heads))
    scores, states = lax.fori_loop(0, r // group, scan_keys, (none_s, none_v))

    probs, new_weights, state_weights, denominators = [], [], [], []
    for h in range(heads):
        log_in = column(g.kv * heads + h) * scale + ins["bi"][h]
        log_forget = log_sigmoid(column(every + g.kv * heads + h) * scale + ins["bf"][h])
        exponent = jnp.where(live, later[h] + log_forget + cached_in[h], -jnp.inf)
        carried = whole_forget[h] + log_forget + ins["stab"][:, h:h + 1]
        most = jnp.maximum(jnp.maximum(jnp.max(exponent, axis=-1, keepdims=True), carried), log_in)
        weight = jnp.exp(exponent - most) * scores[h]
        q_wide = q_of[h].astype(F32)
        new_w = jnp.exp(log_in - most) * jnp.sum(
            q_wide * new_key[:, h * size:(h + 1) * size], axis=-1, keepdims=True
        )
        state_w = jnp.exp(carried - most)
        norm = jnp.sum(ins["nrm"][:, h, :] * q_wide, axis=-1, keepdims=True)
        denominators.append(jnp.sum(weight, axis=-1, keepdims=True) + new_w + state_w * norm)
        probs.append(weight.astype(BF16))
        new_weights.append(new_w)
        state_weights.append(state_w)

    loads["vals"].wait()

    def scan_values(i, carry):
        sums_v = list(carry)
        for j in range(group):
            b = i * group + j
            for h in range(heads):
                s = dot32(probs[h], sc["v_vals"][b, h])
                sums_v[h] = jnp.where(row_v == b, s, sums_v[h])
        return tuple(sums_v)

    block_sums = lax.fori_loop(0, r // group, scan_values, none_v)
    heads_buf = sc["head_buf"]
    for h in range(heads):
        at = slice(h * size, (h + 1) * size)
        numerator = block_sums[h] + new_weights[h] * new_value[:, at] + state_weights[h] * states[h]
        cell = numerator / jnp.maximum(jnp.abs(denominators[h]), 1.0)
        heads_buf[g.t, :, at] = (cell * ins["hgain"][:, at]).astype(BF16)

    head_gather = Gather(g, heads_buf, [sc[f"head_{p}"] for p in ("s", "f", "r")])
    head_gather.run()

    loads["wo"].wait()
    att = dot32(heads_buf[...].reshape(rows, width), sc["v_wo"][...])
    sc["att_sb"][...] = att.astype(BF16).reshape(n_kv, rows // n_kv, feats)
    att_sum = SumOverKv(
        g, sc["att_sb"], sc["att_rb"], sc["att_out"], [sc[f"att_{p}"] for p in ("s1", "r1", "s2", "r2")]
    )
    att_sum.run()
    residual = ins["tokens"][...].astype(F32) + sc["att_out"][...].reshape(rows, feats).astype(F32)
    sc["res"][...] = residual
    sc["mid"][...] = (residual * ins["mgain"][...]).astype(BF16)
    square = jnp.sum(residual * residual, axis=1, keepdims=True)
    sc["msq_sb"][...] = jnp.broadcast_to(square, (rows, 128)).reshape(n_tp, r, 128)

    msq, gate, up = rs("msq"), rs("gate"), rs("up")
    hidden_dev = ins["wg"].shape[1]
    tile = 256

    def project(weight, target):
        if hidden_dev % tile:
            target[...] = dot32(sc["mid"][...], weight[...]).astype(BF16).reshape(n_tp, r, hidden_dev)
            return

        def step(i, _):
            at = pl.ds(pl.multiple_of(i * tile, tile), tile)
            target[:, :, at] = dot32(sc["mid"][...], weight[:, at]).astype(BF16).reshape(n_tp, r, tile)
            return 0

        lax.fori_loop(0, hidden_dev // tile, step, 0)

    loads["wg"].wait()
    project(sc["v_wg"], sc["gate_sb"])
    gate.start()
    msq.start()
    loads["wu"].wait()
    project(sc["v_wu"], sc["up_sb"])
    gate.middle()
    up.start()
    msq.middle()
    up.middle()
    second = lax.rsqrt(msq.end()[:, 0:1] / model + epsilon)
    gate_pre = gate.end() * second
    silu = gate_pre / (1.0 + jnp.exp(-gate_pre))
    hid = (silu * (up.end() * second)).astype(BF16)
    sc["hid_buf"][g.t] = hid
    hid_gather = Gather(g, sc["hid_buf"], [sc[f"hid_{p}"] for p in ("s", "f", "r")])
    hid_gather.run()
    loads["wd"].wait()
    half = feats // 2 if feats % 256 == 0 else feats
    for at in range(0, feats, half):
        part = dot32(sc["hid_buf"][...].reshape(rows, hidden_dev), sc["v_wd"][:, at:at + half])
        sc["ffn_sb"][:, :, at:at + half] = part.astype(BF16).reshape(n_kv, rows // n_kv, half)
    ffn_sum = SumOverKv(
        g, sc["ffn_sb"], sc["ffn_rb"], sc["ffn_out"], [sc[f"ffn_{p}"] for p in ("s1", "r1", "s2", "r2")]
    )
    ffn_sum.run()
    out[...] = sc["res"][...] + sc["ffn_out"][...].reshape(rows, feats).astype(F32)
    for item in (small, qkv, head_gather, att_sum, msq, gate, up, hid_gather, ffn_sum):
        item.drain()


def body(n_tp, n_kv, *args):
    arrays = dict(zip(NAMES, args))
    rows, feats = arrays["tokens"].shape
    r, heads, block, size = arrays["keys"].shape
    width = heads * size
    hidden_dev = arrays["wg"].shape[1]
    nz = n_tp // 2
    for name in ("norm_gain", "hgain", "mgain"):
        arrays[name] = arrays[name].reshape(1, -1)
    dma = pltpu.SemaphoreType.DMA
    scratch = {"v_" + n: pltpu.VMEM(arrays[n].shape, arrays[n].dtype) for n in HELD}
    scratch["load_sem"] = dma((len(HELD),))
    for name, w, dtype in (
        ("small", 128, F32), ("qkv", 3 * width, BF16), ("msq", 128, F32),
        ("gate", hidden_dev, BF16), ("up", hidden_dev, BF16),
    ):
        scratch[name + "_sb"] = pltpu.VMEM((n_tp, r, w), dtype)
        for p in ("rb1", "sb2", "rb2"):
            scratch[f"{name}_{p}"] = pltpu.VMEM((nz, r, w), dtype)
        for p in ("s1", "r1", "s2", "r2"):
            scratch[f"{name}_{p}"] = dma((nz,))
    for name, w in (("head", width), ("hid", hidden_dev)):
        scratch[name + "_buf"] = pltpu.VMEM((n_tp, r, w), BF16)
        scratch[name + "_s"] = dma((nz,))
        scratch[name + "_f"] = dma((nz,))
        scratch[name + "_r"] = dma((n_tp,))
    for name in ("att", "ffn"):
        for p in ("sb", "rb", "out"):
            scratch[f"{name}_{p}"] = pltpu.VMEM((n_kv, rows // n_kv, feats), BF16)
        for p in ("s1", "r1", "s2", "r2"):
            scratch[f"{name}_{p}"] = dma((n_kv,))
    scratch["res"] = pltpu.VMEM((rows, feats), F32)
    scratch["mid"] = pltpu.VMEM((rows, feats), BF16)

    def spec(name):
        if name in HELD:
            return pl.BlockSpec(memory_space=pl.ANY)
        if name in ("bi", "bf", "lens"):
            return pl.BlockSpec(memory_space=pltpu.SMEM)
        return pl.BlockSpec(memory_space=pltpu.VMEM)

    return pl.pallas_call(
        functools.partial(kernel, n_tp, n_kv, feats * n_tp, tuple(scratch)),
        out_shape=jax.ShapeDtypeStruct((rows, feats), F32),
        in_specs=[spec(n) for n in NAMES],
        out_specs=pl.BlockSpec(memory_space=pltpu.VMEM),
        scratch_shapes=list(scratch.values()),
        compiler_params=pltpu.CompilerParams(
            collective_id=0, has_side_effects=True, vmem_limit_bytes=56 * 1024 * 1024
        ),
    )(*[arrays[n] for n in NAMES])


def solution(mesh):
    placed = (
        P(None, "tp"), P("tp"), P("tp", "kv"), P("tp", "kv"), P("tp", "kv"), P("tp", None), P("tp", None),
        P("kv"), P("kv"), P("tp", "kv", None, None), P("tp", "kv", None), P("tp", "kv"),
        P("tp", "kv", None, None), P("tp", "kv", None, None), P("tp", "kv", None), P("tp", "kv", None),
        P("tp"), P("kv"), P("kv", "tp"), P("tp"), P("tp", "kv"), P("tp", "kv"), P("kv", "tp"),
    )
    run = functools.partial(body, mesh.shape["tp"], mesh.shape["kv"])
    return jax.shard_map(run, mesh=mesh, in_specs=placed, out_specs=P(None, "tp"), check_vma=False)
```
